32 devices in a mesh: ep: 16 (over z, y, x), tp: 2 (over core).
Axes of the slice: x: 2, y: 2, z: 4, core: 2. Of those that a mesh axis runs over, the one named last changes fastest.
Arguments:
- inputs: bfloat16 [256, 1536], P('ep'), may hold values from -6 to 6
- norm_gain_attn: float32 [1536], replicated, may hold values from 0.1 to 1.9
- w_query: bfloat16 [1536, 768], P(None, 'tp'), may hold values from -0.15625 to 0.15625
- w_key: bfloat16 [1536, 128], P(None, 'tp'), may hold values from -0.15625 to 0.15625
- w_value: bfloat16 [1536, 128], P(None, 'tp'), may hold values from -0.15625 to 0.15625
- w_forget: bfloat16 [1536, 12], P(None, 'tp'), may hold values from -0.15625 to 0.15625
- forget_bias: float32 [12], P('tp'), may hold values from 0 to 3
- cache_keys: bfloat16 [256, 2, 1024, 64], P('ep', 'tp'), may hold values from -250 to 250
- cache_values: bfloat16 [256, 2, 1024, 64], P('ep', 'tp'), may hold values from -6 to 6
- cache_gates: float32 [256, 12, 1024], P('ep', 'tp'), as said below
- lengths: int32 [256], P('ep'), may hold values from 128 to 1024, as said below
- w_out: bfloat16 [768, 1536], P('tp'), may hold values from -0.21875 to 0.21875
- norm_gain_ffn: float32 [1536], replicated, may hold values from 0.1 to 1.9
- expert_ids: int32 [256, 6], P('ep'), may hold values from 0 to 15, as said below
- group_weights: float32 [256], P('ep'), may hold values from 0.2 to 1
- expert_weights: float32 [256, 6], P('ep'), may hold values from 0.05 to 1
- exp_gate: bfloat16 [16, 1536, 512], P('ep', None, 'tp'), may hold values from -0.15625 to 0.15625
- exp_up: bfloat16 [16, 1536, 512], P('ep', None, 'tp'), may hold values from -0.15625 to 0.15625
- exp_down: bfloat16 [16, 512, 1536], P('ep', 'tp'), may hold values from -0.25 to 0.25
- dense_gate_vector: float32 [1536], replicated, may hold values from -0.15625 to 0.15625
- dense_gate_w: bfloat16 [1536, 16384], P(None, ('ep', 'tp')), may hold values from -0.15625 to 0.15625
- dense_up_w: bfloat16 [1536, 16384], P(None, ('ep', 'tp')), may hold values from -0.15625 to 0.15625
- dense_down_w: bfloat16 [16384, 1536], P(('ep', 'tp')), may hold values from -0.09375 to 0.09375
Outputs:
- mixed: bfloat16 [256, 1536], P('ep', 'tp')
The draws below stay inside these ranges and needn't reach their ends.
Inputs may be any that keep to these rules, and one draw needn't show every extreme that they name: `cache_gates`: Non-increasing along positions. `lengths`: some sequence has 1024. `expert_ids`: each row names 6 different experts that share one group (the same quotient by 8). Among the rows of one index of ep at most 12 name the same expert, and some expert is named by exactly 12 rows of every index of ep.
All inputs are finite; a program needn't handle non-finite values.
Results may differ from the reference program's by a relative error of at most 0.013.
Values may be sent and summed in bfloat16 or wider, within the bound.
A program may use at most 128 MiB of HBM per device.

```python
import jax
import jax.numpy as jnp
from jax import lax

D = 1536
QUERY_HEAD_COUNT = 12
HEAD = 64
KV_HEADS = 2
EXP_FF = 512
EXP_PER_GROUP = 8
TOPK = 6
DENSE_FF = 16384
CACHE_LENGTH = 1024
SEQ_DEV = 16
SEQUENCE_COUNT = 256
EXPERTS = 16
CAP = 12
N_EP = 16


def draw_cache_keys(key, part):
    base = jax.random.normal(jax.random.fold_in(key, 1), (SEQUENCE_COUNT, KV_HEADS, CACHE_LENGTH, HEAD), jnp.float32)
    return base.astype(jnp.bfloat16)


def draw_cache_gates(key, part):
    slow_share = 0.5
    lagging_head = jax.random.uniform(jax.random.fold_in(key, 11), (1, QUERY_HEAD_COUNT, 1), jnp.float32) < slow_share
    slow_rate = jax.random.uniform(jax.random.fold_in(key, 12), (SEQUENCE_COUNT, QUERY_HEAD_COUNT, 1), jnp.float32, 0.3, 1.5) / CACHE_LENGTH
    fast_rate = 1.0 / jax.random.uniform(jax.random.fold_in(key, 13), (SEQUENCE_COUNT, QUERY_HEAD_COUNT, 1), jnp.float32, 30.0, 100.0)
    rates = jnp.where(lagging_head, slow_rate, fast_rate)
    seq_factor = jnp.exp(jax.random.uniform(jax.random.fold_in(key, 14), (SEQUENCE_COUNT, 1, 1), jnp.float32, -0.7, 0.7))
    roughness = jax.random.uniform(jax.random.fold_in(key, 15), (SEQUENCE_COUNT, QUERY_HEAD_COUNT, CACHE_LENGTH), jnp.float32, 0.5, 1.5)
    length_steps = -rates * seq_factor * roughness
    spike_position = jax.random.randint(jax.random.fold_in(key, 16), (SEQUENCE_COUNT, 3), 0, CACHE_LENGTH)
    cache_positions = lax.broadcasted_iota(jnp.int32, (SEQUENCE_COUNT, CACHE_LENGTH), 1)
    spike_mask = jnp.any(cache_positions[:, :, None] == spike_position[:, None, :], axis=2)[:, None, :]
    spike_length = jax.random.uniform(jax.random.fold_in(key, 17), (SEQUENCE_COUNT, QUERY_HEAD_COUNT, CACHE_LENGTH), jnp.float32, 0.22, 0.69)
    length_steps = length_steps - jnp.where(spike_mask & lagging_head, spike_length, 0.0)
    return jnp.cumsum(length_steps, axis=2)


def draw_lengths(key, part):
    counts = jax.random.randint(jax.random.fold_in(key, 21), (SEQUENCE_COUNT,), CACHE_LENGTH // 8, CACHE_LENGTH + 1)
    chosen = jax.random.randint(jax.random.fold_in(key, 22), (), 0, SEQUENCE_COUNT)
    return jnp.where(jnp.arange(SEQUENCE_COUNT) == chosen, CACHE_LENGTH, counts).astype(jnp.int32)


def draw_expert_ids(key, part):
    n_groups = EXPERTS // EXP_PER_GROUP
    main_group = jax.random.randint(jax.random.fold_in(key, 31), (), 0, n_groups)
    main_expert = jax.random.randint(jax.random.fold_in(key, 32), (), 0, EXP_PER_GROUP)

    def one_block(block_key):
        ordering = jax.random.permutation(jax.random.fold_in(block_key, 1), n_groups)
        labels = (ordering - ordering[0] + main_group) % n_groups
        pool = jnp.repeat(labels, CAP)
        others = jax.random.permutation(jax.random.fold_in(block_key, 2), pool[CAP:])
        block_groups = jnp.concatenate([pool[:CAP], others])[:SEQ_DEV]
        token_order = jax.random.permutation(jax.random.fold_in(block_key, 3), SEQ_DEV)
        groups_here = block_groups[token_order]
        forced = token_order < CAP
        scores = jax.random.randint(jax.random.fold_in(block_key, 4), (SEQ_DEV, EXP_PER_GROUP), 0, 1 << 20) * EXP_PER_GROUP + jnp.arange(EXP_PER_GROUP)[None, :]
        ranking = jnp.argsort(scores, axis=1)
        picked = ranking[:, :TOPK]
        present = jnp.any(picked == main_expert, axis=1)
        replaced = picked.at[:, 0].set(main_expert)
        picked = jnp.where((forced & ~present)[:, None], replaced, picked)
        return groups_here[:, None] * EXP_PER_GROUP + picked
    block_keys = jax.random.split(jax.random.fold_in(key, 33), N_EP)
    return jax.vmap(one_block)(block_keys).reshape(SEQUENCE_COUNT, TOPK).astype(jnp.int32)


def level_of(key, dims, pieces, least, high):
    def one(position, shards_of):
        steps = jax.random.uniform(jax.random.fold_in(jax.random.fold_in(key, 6), position), (shards_of,), jnp.float32, least / len(pieces), high / len(pieces))
        return jnp.repeat(jnp.exp(steps), dims[position] // shards_of).reshape((-1,) + (1,) * (len(dims) - position - 1))

    level = one(*pieces[0])
    for cut in pieces[1:]:
        level = level * one(*cut)
    return level


def normal_values(own_key, extent, spread, bound, cuts=(), held_as=jnp.bfloat16):
    values = spread * jax.random.normal(own_key, extent, jnp.float32)
    if cuts:
        values = values * level_of(own_key, extent, cuts, -0.22, 0.18)
    return jnp.clip(values, -bound, bound).astype(held_as)


def setup_inputs(seed: int = 0) -> dict:
    seeds = jax.random.split(jax.random.key(seed), 24)
    return {
        "inputs": normal_values(seeds[0], (SEQUENCE_COUNT, D), 1.0, 6.0, ((0, 16),)),
        "norm_gain_attn": jnp.clip(1.0 + 0.18 * jax.random.normal(seeds[1], (D,), jnp.float32), 0.1, 1.9),
        "w_query": normal_values(seeds[2], (D, QUERY_HEAD_COUNT * HEAD), D ** -0.5, 0.15625, ((1, 2),)),
        "w_key": normal_values(seeds[3], (D, KV_HEADS * HEAD), D ** -0.5, 0.15625, ((1, 2),)),
        "w_value": normal_values(seeds[4], (D, KV_HEADS * HEAD), D ** -0.5, 0.15625, ((1, 2),)),
        "w_forget": normal_values(seeds[5], (D, QUERY_HEAD_COUNT), D ** -0.5, 0.15625, ((1, 2),)),
        "forget_bias": jnp.clip(3.0 * jax.random.uniform(seeds[6], (QUERY_HEAD_COUNT,), jnp.float32) ** level_of(seeds[6], (QUERY_HEAD_COUNT,), ((0, 2),), -0.2, 0.2), 0.0, 3.0),
        "cache_keys": draw_cache_keys(jax.random.fold_in(seeds[23], 71), 0),
        "cache_values": normal_values(seeds[8], (SEQUENCE_COUNT, KV_HEADS, CACHE_LENGTH, HEAD), 1.0, 6.0, ((0, 16), (1, 2))),
        "cache_gates": draw_cache_gates(jax.random.fold_in(seeds[23], 71), 0),
        "lengths": draw_lengths(jax.random.fold_in(seeds[23], 71), 0),
        "w_out": normal_values(seeds[11], (QUERY_HEAD_COUNT * HEAD, D), (QUERY_HEAD_COUNT * HEAD) ** -0.5, 0.21875, ((0, 2),)),
        "norm_gain_ffn": jnp.clip(1.0 + 0.18 * jax.random.normal(seeds[12], (D,), jnp.float32), 0.1, 1.9),
        "expert_ids": draw_expert_ids(jax.random.fold_in(seeds[23], 71), 0),
        "group_weights": jnp.clip(0.2 + 0.8 * jax.random.uniform(seeds[14], (SEQUENCE_COUNT,), jnp.float32) ** level_of(seeds[14], (SEQUENCE_COUNT,), ((0, 16),), -0.2, 0.2), 0.2, 1.0),
        "expert_weights": jnp.clip(0.05 + 0.95 * jax.random.uniform(seeds[15], (SEQUENCE_COUNT, TOPK), jnp.float32) ** level_of(seeds[15], (SEQUENCE_COUNT, TOPK), ((0, 16),), -0.2, 0.2), 0.05, 1.0),
        "exp_gate": normal_values(seeds[16], (EXPERTS, D, EXP_FF), D ** -0.5, 0.15625, ((0, 16), (2, 2))),
        "exp_up": normal_values(seeds[17], (EXPERTS, D, EXP_FF), D ** -0.5, 0.15625, ((0, 16), (2, 2))),
        "exp_down": normal_values(seeds[18], (EXPERTS, EXP_FF, D), EXP_FF ** -0.5, 0.25, ((0, 16), (1, 2))),
        "dense_gate_vector": normal_values(seeds[19], (D,), D ** -0.5, 0.15625, (), jnp.float32),
        "dense_gate_w": normal_values(seeds[20], (D, DENSE_FF), D ** -0.5, 0.15625, ((1, 32),)),
        "dense_up_w": normal_values(seeds[21], (D, DENSE_FF), D ** -0.5, 0.15625, ((1, 32),)),
        "dense_down_w": normal_values(seeds[22], (DENSE_FF, D), (DENSE_FF // 4) ** -0.5, 0.09375, ((0, 32),)),
    }


EPS = 1e-06

def rounded(values):
    return lax.optimization_barrier(values.astype(jnp.bfloat16)).astype(jnp.float32)

def rms_scale(row_block, gain):
    row_block = row_block.astype(jnp.float32)
    factor = lax.rsqrt(lax.optimization_barrier(jnp.mean(row_block * row_block, axis=-1, keepdims=True)) + EPS)
    return (row_block * factor * gain).astype(jnp.bfloat16)

def attend(bundle):
    queries, new_key, new_value, log_forget, keys, values, gates, counts = bundle
    seqs_here, kv_count, group_size, head_size = queries.shape
    cache_positions = lax.broadcasted_iota(jnp.int32, (1, 1, gates.shape[2]), 2)
    last_gate = lax.optimization_barrier(jnp.sum(jnp.where(cache_positions == (counts - 1)[:, None, None], gates, 0.0), axis=2))
    offsets = (last_gate + log_forget)[:, :, None] - gates
    offsets = offsets.reshape(seqs_here, kv_count, group_size, gates.shape[2])
    scale_factor = head_size ** (-0.5)
    query_wide = queries.astype(jnp.float32)
    cached = jnp.einsum('skgd,skld->skgl', query_wide, keys.astype(jnp.float32)) * scale_factor + offsets
    valid_mask = cache_positions.reshape(1, 1, 1, -1) < counts[:, None, None, None]
    cached = jnp.where(valid_mask, cached, -jnp.inf)
    own_score = lax.optimization_barrier(jnp.sum(query_wide * new_key.astype(jnp.float32)[:, :, None, :], axis=3)) * scale_factor
    peak_score = jnp.maximum(lax.optimization_barrier(jnp.max(cached, axis=3)), own_score)
    cached_exp = jnp.exp(cached - peak_score[..., None])
    own_exp = jnp.exp(own_score - peak_score)
    denominator = lax.optimization_barrier(jnp.sum(cached_exp, axis=3)) + own_exp
    cached_weight = (cached_exp / denominator[..., None]).astype(jnp.bfloat16)
    own_weight = (own_exp / denominator).astype(jnp.bfloat16)
    mixed_values = jnp.einsum('skgl,skld->skgd', cached_weight.astype(jnp.float32), values.astype(jnp.float32))
    mixed_values = mixed_values + own_weight.astype(jnp.float32)[..., None] * new_value.astype(jnp.float32)[:, :, None, :]
    return mixed_values.reshape(seqs_here, kv_count * group_size * head_size).astype(jnp.bfloat16)

def run_expert(bundle):
    row_block, gate_weight, up_weight, down_weight = bundle
    gate_part = jnp.dot(row_block, gate_weight, preferred_element_type=jnp.float32)
    up_part = jnp.dot(row_block, up_weight, preferred_element_type=jnp.float32)
    activated = (jax.nn.silu(gate_part) * up_part).astype(jnp.bfloat16)
    half_units = activated.shape[1] // 2
    first_part = rounded(jnp.dot(activated[:, :half_units], down_weight[:half_units], preferred_element_type=jnp.float32))
    second_part = rounded(jnp.dot(activated[:, half_units:], down_weight[half_units:], preferred_element_type=jnp.float32))
    return (first_part + second_part).astype(jnp.bfloat16)

def reference(inputs, norm_gain_attn, w_query, w_key, w_value, w_forget, forget_bias, cache_keys, cache_values, cache_gates, lengths, w_out, norm_gain_ffn, expert_ids, group_weights, expert_weights, exp_gate, exp_up, exp_down, dense_gate_vector, dense_gate_w, dense_up_w, dense_down_w):
    normed = rms_scale(inputs, norm_gain_attn)
    group_size = QUERY_HEAD_COUNT // KV_HEADS
    queries = jnp.dot(normed, w_query, preferred_element_type=jnp.float32).astype(jnp.bfloat16)
    new_keys = jnp.dot(normed, w_key, preferred_element_type=jnp.float32).astype(jnp.bfloat16)
    new_values = jnp.dot(normed, w_value, preferred_element_type=jnp.float32).astype(jnp.bfloat16)
    log_forget = jax.nn.log_sigmoid(jnp.dot(normed, w_forget, preferred_element_type=jnp.float32) + forget_bias)
    bundle = (queries.reshape(N_EP, SEQ_DEV, KV_HEADS, group_size, HEAD), new_keys.reshape(N_EP, SEQ_DEV, KV_HEADS, HEAD), new_values.reshape(N_EP, SEQ_DEV, KV_HEADS, HEAD), log_forget.reshape(N_EP, SEQ_DEV, QUERY_HEAD_COUNT), cache_keys.reshape(N_EP, SEQ_DEV, KV_HEADS, CACHE_LENGTH, HEAD), cache_values.reshape(N_EP, SEQ_DEV, KV_HEADS, CACHE_LENGTH, HEAD), cache_gates.reshape(N_EP, SEQ_DEV, QUERY_HEAD_COUNT, CACHE_LENGTH), lengths.reshape(N_EP, SEQ_DEV))
    heads_out = lax.map(attend, bundle).reshape(SEQUENCE_COUNT, QUERY_HEAD_COUNT * HEAD)
    half_heads = QUERY_HEAD_COUNT * HEAD // 2
    attn_out = rounded(jnp.dot(heads_out[:, :half_heads], w_out[:half_heads], preferred_element_type=jnp.float32))
    attn_out = attn_out + rounded(jnp.dot(heads_out[:, half_heads:], w_out[half_heads:], preferred_element_type=jnp.float32))
    after_attn = inputs.astype(jnp.float32) + attn_out
    normed_ffn = rms_scale(after_attn, norm_gain_ffn)
    flat_ids = expert_ids.reshape(-1).astype(jnp.int32)
    hit_table = (flat_ids[:, None] == jnp.arange(EXPERTS, dtype=jnp.int32)[None, :]).astype(jnp.int32)
    hit_blocks = hit_table.reshape(N_EP, SEQ_DEV * TOPK, EXPERTS)
    earlier = (jnp.cumsum(hit_blocks, axis=1) - hit_blocks).reshape(SEQUENCE_COUNT * TOPK, EXPERTS)
    slot_rank = lax.optimization_barrier(jnp.sum(earlier * hit_table, axis=1))
    source = jnp.arange(SEQUENCE_COUNT * TOPK, dtype=jnp.int32) // (SEQ_DEV * TOPK)
    slot_index = (source * CAP + slot_rank).astype(jnp.int32)
    repeated = jnp.repeat(normed_ffn, TOPK, axis=0)
    dispatched = jnp.zeros((EXPERTS, N_EP * CAP, D), jnp.bfloat16).at[flat_ids, slot_index].set(repeated)
    expert_rows = lax.map(run_expert, (dispatched, exp_gate, exp_up, exp_down))
    picked_rows = expert_rows[flat_ids, slot_index].astype(jnp.float32)
    route_weight = (group_weights[:, None] * expert_weights).reshape(SEQUENCE_COUNT * TOPK, 1)
    expert_mix = lax.optimization_barrier(jnp.sum((picked_rows * route_weight).reshape(SEQUENCE_COUNT, TOPK, D), axis=1))
    dense_gate = jnp.dot(normed_ffn, dense_gate_w, preferred_element_type=jnp.float32)
    dense_up = jnp.dot(normed_ffn, dense_up_w, preferred_element_type=jnp.float32)
    dense_hidden = (jax.nn.silu(dense_gate) * dense_up).astype(jnp.bfloat16)
    dense_out = jnp.dot(dense_hidden, dense_down_w, preferred_element_type=jnp.float32)
    gating = jax.nn.sigmoid(jnp.dot(normed_ffn.astype(jnp.float32), dense_gate_vector, precision=lax.Precision.HIGHEST))
    return (after_attn + expert_mix + gating[:, None] * dense_out).astype(jnp.bfloat16)
```

```python
import functools

import jax
import jax.numpy as jnp
from jax import lax
from jax.experimental import pallas as pl
from jax.experimental.pallas import tpu as pltpu
from jax.sharding import PartitionSpec as P

EPS = 1e-06


def rms_scale(row_block, gain):
    row_block = row_block.astype(jnp.float32)
    factor = lax.rsqrt(jnp.mean(row_block * row_block, axis=-1, keepdims=True) + EPS)
    return (row_block * factor * gain).astype(jnp.bfloat16)


MESH = pl.DeviceIdType.MESH


def layer_kernel(
    n,
    plane,
    inp_h,
    gain_a_h,
    wq_h,
    wk_h,
    wv_h,
    wf_h,
    bias_h,
    keys_h,
    vals_h,
    gates_h,
    lens_h,
    gain_h,
    dgv_h,
    ids_h,
    group_weight_h,
    expert_weight_h,
    wo,
    wg,
    wu,
    wd,
    eg,
    eu,
    ed,
    out,
    inp,
    gain_a,
    wq_v,
    wkv_v,
    wf_v,
    bias,
    keys_v,
    vals_v,
    gates_v,
    lens,
    gain,
    dgv,
    ids,
    group_weight,
    expert_weight,
    spread_q,
    score,
    weight_v,
    mixed_v,
    wo_v,
    wg_v,
    wu_v,
    wd_v,
    eg_v,
    eu_v,
    ed_v,
    xbuf,
    part,
    pbuf,
    aft,
    hid_d,
    hid_e,
    to_pair,
    from_pair,
    own,
    rs_send,
    rs_buf,
    line_send,
    line_buf,
    in_sem,
    w_sem,
    pair_sem,
    ag_s,
    ag_r,
    fw_s,
    fw_r,
    rs_s,
    rs_r,
    zag_s,
    zrs_s,
    zrs_r,
):
    me = lax.axis_index("ep")
    depth = n // plane
    z = lax.div(me, plane)
    p = lax.rem(me, plane)
    direction = 1 - 2 * lax.div(2 * z, depth)
    c = lax.axis_index("tp")
    other = 1 - c
    rows, width = inp.shape
    half = width // 2
    total = xbuf.shape[1]
    local_experts = eg.shape[0]
    n_experts = n * local_experts

    loads = [
        pltpu.make_async_copy(hbm, vmem, w_sem.at[i])
        for i, (hbm, vmem) in enumerate(
            ((wo, wo_v), (wg, wg_v), (wu, wu_v), (eg, eg_v), (eu, eu_v), (wd, wd_v), (ed, ed_v))
        )
    ]
    head_size = wk_h.shape[0]
    small = (
        (inp_h, inp),
        (gain_a_h, gain_a),
        (wq_h, wq_v),
        (wk_h, wkv_v.at[:head_size]),
        (wv_h, wkv_v.at[head_size:]),
        (wf_h, wf_v),
        (bias_h, bias),
        (lens_h, lens),
        (gates_h, gates_v),
        (keys_h, keys_v),
        (vals_h, vals_v),
        (gain_h, gain),
        (dgv_h, dgv),
        (ids_h, ids),
        (group_weight_h, group_weight),
        (expert_weight_h, expert_weight),
    )
    brings = [
        pltpu.make_async_copy(hbm, vmem, in_sem.at[i]) for i, (hbm, vmem) in enumerate(small)
    ]
    for bring in brings:
        bring.start()
    for load in loads:
        load.start()

    barrier = pltpu.get_barrier_semaphore()
    pl.semaphore_signal(barrier, inc=1, device_id={"tp": other}, device_id_type=MESH)

    def line_peer(s):
        return lax.rem(z + direction * s + depth, depth)

    def plane_peer(s):
        return lax.rem(p + s, plane)

    def greet_line(s, carry):
        pl.semaphore_signal(
            barrier, inc=1, device_id={"ep": line_peer(s) * plane + p}, device_id_type=MESH
        )
        return carry

    def greet_plane(s, carry):
        pl.semaphore_signal(
            barrier, inc=1, device_id={"ep": z * plane + plane_peer(s)}, device_id_type=MESH
        )
        return carry

    lax.fori_loop(1, depth, greet_line, 0)
    lax.fori_loop(1, plane, greet_plane, 0)

    side_width = xbuf.shape[2] - half
    lanes = lax.broadcasted_iota(jnp.int32, (rows, side_width), 1)
    row_index = lax.broadcasted_iota(jnp.int32, (rows, rows), 0)
    column_index = lax.broadcasted_iota(jnp.int32, (rows, rows), 1)
    diagonal = row_index == column_index

    def column(row):
        return jnp.sum(jnp.where(diagonal, row, 0.0), axis=1, keepdims=True)

    for bring in brings[:8]:
        bring.wait()
    normed = rms_scale(inp[...], gain_a[...][None, :])
    nt = (((1,), (1,)), ((), ()))
    queries = jnp.dot(normed, wq_v[...], preferred_element_type=jnp.float32)
    new_kv = lax.dot_general(normed, wkv_v[...], nt, preferred_element_type=jnp.float32)
    forget = lax.dot_general(normed, wf_v[...], nt, preferred_element_type=jnp.float32)
    forget = forget + bias[...][None, :]
    forget = jnp.minimum(forget, 0.0) - jnp.log1p(jnp.exp(-jnp.abs(forget)))
    queries = queries.astype(jnp.bfloat16).astype(jnp.float32)
    new_kv = new_kv.astype(jnp.bfloat16).astype(jnp.float32)
    kv_swapped = pltpu.roll(new_kv, head_size, 1)
    pair_lane = lax.broadcasted_iota(jnp.int32, new_kv.shape, 1)
    first = pair_lane < head_size
    new_key = jnp.where(first, new_kv, kv_swapped)
    new_value = jnp.where(first, kv_swapped, new_kv)
    span = rows * head_size
    own_block = lax.div(
        lax.broadcasted_iota(jnp.int32, (rows, span), 1), head_size
    ) == lax.broadcasted_iota(jnp.int32, (rows, span), 0)
    head_count = wf_h.shape[0]
    lanes_pair = 2 * head_size
    own_scores = []
    scale_factor = head_size ** (-0.5)
    for h in range(head_count):
        pair = queries[:, (h // 2) * lanes_pair : (h // 2 + 1) * lanes_pair]
        swapped = pltpu.roll(pair, head_size, 1)
        doubled = jnp.where(first, pair, swapped) if h % 2 == 0 else jnp.where(first, swapped, pair)
        own_scores.append(
            jnp.sum(jnp.where(first, doubled * new_key, 0.0), axis=1, keepdims=True) * scale_factor
        )
        wide = jnp.concatenate([doubled] * (span // lanes_pair), axis=1)
        spread_q[h * rows : (h + 1) * rows, :] = jnp.where(own_block, wide, 0.0).astype(
            jnp.bfloat16
        )
    for bring in brings[8:10]:
        bring.wait()
    score[...] = jnp.dot(spread_q[...], keys_v[...], preferred_element_type=jnp.float32)
    counts = column(lens[...][None, :].astype(jnp.float32)).astype(jnp.int32)
    positions = lax.broadcasted_iota(jnp.int32, (rows, gates_v.shape[2]), 1)
    own_weights = []
    for h in range(head_count):
        gates = gates_v[h]
        last = jnp.sum(jnp.where(positions == counts - 1, gates, 0.0), axis=1, keepdims=True)
        offsets = (last + forget[:, h : h + 1]) - gates
        cached = score[h * rows : (h + 1) * rows, :] * scale_factor + offsets
        cached = jnp.where(positions < counts, cached, -jnp.inf)
        peak = jnp.maximum(jnp.max(cached, axis=1, keepdims=True), own_scores[h])
        cached = jnp.exp(cached - peak)
        own_exp = jnp.exp(own_scores[h] - peak)
        inverse = 1.0 / (jnp.sum(cached, axis=1, keepdims=True) + own_exp)
        weight_v[h * rows : (h + 1) * rows, :] = (cached * inverse).astype(jnp.bfloat16)
        own_weights.append((own_exp * inverse).astype(jnp.bfloat16).astype(jnp.float32))
    brings[10].wait()
    mixed_v[...] = lax.dot_general(
        weight_v[...], vals_v[...], nt, preferred_element_type=jnp.float32
    )
    folded = []
    for h in range(head_count):
        block_values = jnp.where(own_block, mixed_v[h * rows : (h + 1) * rows, :], 0.0)
        total_pair = block_values[:, :lanes_pair]
        for k in range(1, span // lanes_pair):
            total_pair += block_values[:, k * lanes_pair : (k + 1) * lanes_pair]
        total_pair += pltpu.roll(total_pair, head_size, 1)
        folded.append(total_pair + own_weights[h] * new_value)
    heads = jnp.concatenate(
        [jnp.where(first, folded[h], folded[h + 1]) for h in range(0, head_count, 2)], axis=1
    ).astype(jnp.bfloat16)
    for bring in brings[11:]:
        bring.wait()

    group = group_weight[...][None, :]
    lane_values = lanes.astype(jnp.float32)
    route = jnp.zeros((rows, side_width), jnp.float32)
    for k in range(ids.shape[0]):
        choice = column(ids[k : k + 1, :].astype(jnp.float32))
        weight = column(group * expert_weight[k : k + 1, :])
        route = jnp.where(lane_values == choice, weight, route)

    loads[0].wait()
    part[...] = jnp.dot(heads, wo_v[...], preferred_element_type=jnp.float32).astype(
        jnp.bfloat16
    )
    pl.semaphore_wait(barrier, depth + plane - 1)

    swap = pltpu.make_async_remote_copy(
        src_ref=part,
        dst_ref=pbuf,
        send_sem=pair_sem.at[0],
        recv_sem=pair_sem.at[1],
        device_id={"tp": other},
        device_id_type=MESH,
    )
    swap.start()
    swap.wait_recv()

    after = inp[...].astype(jnp.float32) + (
        part[...].astype(jnp.float32) + pbuf[...].astype(jnp.float32)
    )
    aft[...] = after
    factor = lax.rsqrt(jnp.mean(after * after, axis=-1, keepdims=True) + EPS)
    normed = (after * factor * gain[...][None, :]).astype(jnp.bfloat16)
    logit = jnp.sum(normed.astype(jnp.float32) * dgv[...][None, :], axis=-1, keepdims=True)
    gating = 1.0 / (1.0 + jnp.exp(-logit))
    side = jnp.where(lanes == n_experts, gating, route)
    side_high = side.astype(jnp.bfloat16)
    side_low = (side - side_high.astype(jnp.float32)).astype(jnp.bfloat16)

    def block(j):
        return pl.ds(pl.multiple_of(j * rows, rows), rows)

    xbuf[0, block(me), :half] = normed[:, :half]
    xbuf[1, block(me), :half] = normed[:, half:]
    xbuf[0, block(me), half:] = side_high
    xbuf[1, block(me), half:] = side_low

    def line_copy(source, target):
        index = source * plane + p
        return pltpu.make_async_remote_copy(
            src_ref=xbuf.at[c, block(index)],
            dst_ref=xbuf.at[c, block(index)],
            send_sem=zag_s.at[target],
            recv_sem=ag_r.at[index],
            device_id={"ep": target * plane + p},
            device_id_type=MESH,
        )

    def plane_copy(level, source, target):
        index = level * plane + source
        return pltpu.make_async_remote_copy(
            src_ref=xbuf.at[c, block(index)],
            dst_ref=xbuf.at[c, block(index)],
            send_sem=ag_s.at[level * plane + target],
            recv_sem=ag_r.at[index],
            device_id={"ep": z * plane + target},
            device_id_type=MESH,
        )

    def forward_copy(source, part_index):
        return pltpu.make_async_remote_copy(
            src_ref=xbuf.at[part_index, block(source)],
            dst_ref=xbuf.at[part_index, block(source)],
            send_sem=fw_s.at[source],
            recv_sem=fw_r.at[source],
            device_id={"tp": other},
            device_id_type=MESH,
        )

    def spread_plane(level):
        def body(s, carry):
            plane_copy(level, p, plane_peer(s)).start()
            return carry

        lax.fori_loop(1, plane, body, 0)

    def spread_line(s, carry):
        line_copy(z, line_peer(s)).start()
        return carry

    lax.fori_loop(1, depth, spread_line, 0)
    spread_plane(z)

    def pass_on(s, carry):
        level = line_peer(s)
        line_copy(level, z).wait_recv()
        spread_plane(level)
        forward_copy(level * plane + p, c).start()
        return carry

    lax.fori_loop(1, depth, pass_on, 0)

    def take_plane(t, carry):
        level = line_peer(lax.div(t, plane - 1))
        source = plane_peer(1 + lax.rem(t, plane - 1))
        plane_copy(level, source, p).wait_recv()
        forward_copy(level * plane + source, c).start()
        return carry

    lax.fori_loop(0, depth * (plane - 1), take_plane, 0)

    for load in loads[1:5]:
        load.wait()

    def arrive(s, carry):
        forward_copy(lax.rem(me + n - s, n), other).wait_recv()
        return carry

    lax.fori_loop(1, n, arrive, 0)

    chunk = min(total, 256)

    def pick(values, lane):
        index = lax.broadcasted_iota(jnp.int32, values.shape, 1)
        return jnp.sum(jnp.where(index == lane, values, 0.0), axis=1, keepdims=True)

    def dot(a, b):
        return jnp.dot(a, b, preferred_element_type=jnp.float32)

    def hidden(q, carry):
        at = pl.ds(pl.multiple_of(q * chunk, chunk), chunk)
        x0 = xbuf[0, at, :half]
        x1 = xbuf[1, at, :half]
        sides = xbuf[0, at, half:].astype(jnp.float32) + xbuf[1, at, half:].astype(jnp.float32)
        gate = dot(x0, wg_v[:half]) + dot(x1, wg_v[half:])
        up = dot(x0, wu_v[:half]) + dot(x1, wu_v[half:])
        hid_d[at, :] = (gate / (1.0 + jnp.exp(-gate)) * up * pick(sides, n_experts)).astype(
            jnp.bfloat16
        )
        for e in range(local_experts):
            gate = dot(x0, eg_v[e, :half]) + dot(x1, eg_v[e, half:])
            up = dot(x0, eu_v[e, :half]) + dot(x1, eu_v[e, half:])
            weight = pick(sides, me * local_experts + e)
            hid_e[e, at, :] = (gate / (1.0 + jnp.exp(-gate)) * up * weight).astype(jnp.bfloat16)
        return carry

    def down(at, side_index):
        columns = pl.ds(pl.multiple_of(side_index * half, 128), half)
        result = dot(hid_d[at, :], wd_v[:, columns])
        for e in range(local_experts):
            result += dot(hid_e[e, at, :], ed_v[e, :, columns])
        return result

    def down_pair(q, carry):
        at = pl.ds(pl.multiple_of(q * chunk, chunk), chunk)
        to_pair[at, :] = down(at, other).astype(jnp.bfloat16)
        return carry

    def down_own(q, carry):
        at = pl.ds(pl.multiple_of(q * chunk, chunk), chunk)
        own[at, :] = down(at, c)
        return carry

    def combine(q, carry):
        at = pl.ds(pl.multiple_of(q * chunk, chunk), chunk)
        rs_send[at, :] = (own[at, :] + from_pair[at, :].astype(jnp.float32)).astype(jnp.bfloat16)
        return carry

    chunks = total // chunk
    lax.fori_loop(0, chunks, hidden, 0)
    for load in loads[5:]:
        load.wait()
    lax.fori_loop(0, chunks, down_pair, 0)
    trade = pltpu.make_async_remote_copy(
        src_ref=to_pair,
        dst_ref=from_pair,
        send_sem=pair_sem.at[2],
        recv_sem=pair_sem.at[3],
        device_id={"tp": other},
        device_id_type=MESH,
    )
    trade.start()
    lax.fori_loop(0, chunks, down_own, 0)
    trade.wait_recv()
    lax.fori_loop(0, chunks, combine, 0)

    def share_copy(level, source, target):
        return pltpu.make_async_remote_copy(
            src_ref=rs_send.at[block(level * plane + target)],
            dst_ref=rs_buf.at[block(level * plane + source)],
            send_sem=rs_s.at[level * plane + target],
            recv_sem=rs_r.at[level * plane + source],
            device_id={"ep": z * plane + target},
            device_id_type=MESH,
        )

    def settle_copy(source, target):
        return pltpu.make_async_remote_copy(
            src_ref=line_send.at[block(target)],
            dst_ref=line_buf.at[block(source)],
            send_sem=zrs_s.at[target],
            recv_sem=zrs_r.at[source],
            device_id={"ep": target * plane + p},
            device_id_type=MESH,
        )

    def share(t, carry):
        level = line_peer(depth - 1 - lax.div(t, plane - 1))
        share_copy(level, p, plane_peer(1 + lax.rem(t, plane - 1))).start()
        return carry

    lax.fori_loop(0, depth * (plane - 1), share, 0)

    def plane_sum(level):
        index = level * plane + p
        start = own[block(index), :] + from_pair[block(index), :].astype(jnp.float32)

        def body(s, acc):
            source = plane_peer(s)
            share_copy(level, source, p).wait_recv()
            return acc + rs_buf[block(level * plane + source), :].astype(jnp.float32)

        return lax.fori_loop(1, plane, body, start)

    def settle(s, carry):
        level = line_peer(depth - s)
        line_send[block(level), :] = plane_sum(level).astype(jnp.bfloat16)
        settle_copy(z, level).start()
        return carry

    lax.fori_loop(1, depth, settle, 0)
    columns = pl.ds(pl.multiple_of(c * half, 128), half)
    summed = plane_sum(z) + aft[:, columns]

    def collect(s, acc):
        level = line_peer(s)
        settle_copy(level, z).wait_recv()
        return acc + line_buf[block(level), :].astype(jnp.float32)

    summed = lax.fori_loop(1, depth, collect, summed)
    out[...] = summed.astype(out.dtype)

    swap.wait_send()
    trade.wait_send()

    def finish_line(s, carry):
        peer = line_peer(s)
        line_copy(z, peer).wait_send()
        settle_copy(z, peer).wait_send()
        return carry

    def finish_plane(t, carry):
        level = line_peer(lax.div(t, plane - 1))
        target = plane_peer(1 + lax.rem(t, plane - 1))
        plane_copy(level, p, target).wait_send()
        share_copy(level, p, target).wait_send()
        return carry

    def finish_forward(s, carry):
        forward_copy(lax.rem(me + s, n), c).wait_send()
        return carry

    lax.fori_loop(1, depth, finish_line, 0)
    lax.fori_loop(0, depth * (plane - 1), finish_plane, 0)
    lax.fori_loop(1, n, finish_forward, 0)


def layer(n, *operands):
    inputs, _, wq, wk, _, wf, bias, keys, _, gates, lens = operands[:11]
    _, dgv, ids, group_weight, expert_weight, wo, wg, wu, wd, eg, eu, ed = operands[11:]
    rows, width = inputs.shape
    half = width // 2
    total = n * rows
    plane = 1
    while plane * plane < n:
        plane *= 2
    side_width = (n * eg.shape[0] + 128) // 128 * 128
    dense = wg.shape[1]
    local_experts, _, expert_ff = eg.shape
    head_count, _, cache = gates.shape
    head_size = wk.shape[0]
    bf16, f32 = jnp.bfloat16, jnp.float32
    vmem = pl.BlockSpec(memory_space=pltpu.VMEM)
    hbm = pl.BlockSpec(memory_space=pl.ANY)
    dma = pltpu.SemaphoreType.DMA

    def like(array):
        return pltpu.VMEM(array.shape, array.dtype)

    return pl.pallas_call(
        functools.partial(layer_kernel, n, plane),
        out_shape=jax.ShapeDtypeStruct((rows, half), bf16),
        in_specs=[hbm] * len(operands),
        out_specs=vmem,
        scratch_shapes=[
            like(inputs),
            like(dgv),
            like(wq),
            pltpu.VMEM((2 * head_size, width), bf16),
            like(wf),
            like(bias),
            like(keys),
            like(keys),
            like(gates),
            like(lens),
            like(dgv),
            like(dgv),
            like(ids),
            like(group_weight),
            like(expert_weight),
            pltpu.VMEM((head_count * rows, rows * head_size), bf16),
            pltpu.VMEM((head_count * rows, cache), f32),
            pltpu.VMEM((head_count * rows, cache), bf16),
            pltpu.VMEM((head_count * rows, rows * head_size), f32),
            pltpu.VMEM(wo.shape, bf16),
            pltpu.VMEM(wg.shape, bf16),
            pltpu.VMEM(wu.shape, bf16),
            pltpu.VMEM(wd.shape, bf16),
            pltpu.VMEM(eg.shape, bf16),
            pltpu.VMEM(eu.shape, bf16),
            pltpu.VMEM(ed.shape, bf16),
            pltpu.VMEM((2, total, half + side_width), bf16),
            pltpu.VMEM((rows, width), bf16),
            pltpu.VMEM((rows, width), bf16),
            pltpu.VMEM((rows, width), f32),
            pltpu.VMEM((total, dense), bf16),
            pltpu.VMEM((local_experts, total, expert_ff), bf16),
            pltpu.VMEM((total, half), bf16),
            pltpu.VMEM((total, half), bf16),
            pltpu.VMEM((total, half), f32),
            pltpu.VMEM((total, half), bf16),
            pltpu.VMEM((total, half), bf16),
            pltpu.VMEM((n // plane * rows, half), bf16),
            pltpu.VMEM((n // plane * rows, half), bf16),
            dma((16,)),
            dma((7,)),
            dma((4,)),
            dma((n,)),
            dma((n,)),
            dma((n,)),
            dma((n,)),
            dma((n,)),
            dma((n,)),
            dma((n // plane,)),
            dma((n // plane,)),
            dma((n // plane,)),
        ],
        compiler_params=pltpu.CompilerParams(
            collective_id=0, has_side_effects=True, vmem_limit_bytes=56 * 1024 * 1024
        ),
    )(*operands)


def stacked(cache):
    flipped = jnp.swapaxes(cache, 2, 3)
    return flipped.reshape(-1, flipped.shape[3])


def shards(
    inputs,
    norm_gain_attn,
    w_query,
    w_key,
    w_value,
    w_forget,
    forget_bias,
    cache_keys,
    cache_values,
    cache_gates,
    lengths,
    w_out,
    norm_gain_ffn,
    expert_ids,
    group_weights,
    expert_weights,
    exp_gate,
    exp_up,
    exp_down,
    dense_gate_vector,
    dense_gate_w,
    dense_up_w,
    dense_down_w,
):
    return layer(
        lax.axis_size("ep"),
        inputs,
        norm_gain_attn,
        w_query,
        w_key.T,
        w_value.T,
        w_forget.T,
        forget_bias,
        stacked(cache_keys),
        stacked(cache_values),
        jnp.swapaxes(cache_gates, 0, 1),
        lengths,
        norm_gain_ffn,
        dense_gate_vector,
        expert_ids.T,
        group_weights,
        expert_weights.T,
        w_out,
        dense_gate_w,
        dense_up_w,
        dense_down_w,
        exp_gate,
        exp_up,
        exp_down,
    )


def solution(mesh):
    placed = (
        P("ep", None),
        P(),
        P(None, "tp"),
        P(None, "tp"),
        P(None, "tp"),
        P(None, "tp"),
        P("tp"),
        P("ep", "tp", None, None),
        P("ep", "tp", None, None),
        P("ep", "tp", None),
        P("ep"),
        P("tp", None),
        P(),
        P("ep", None),
        P("ep"),
        P("ep", None),
        P("ep", None, "tp"),
        P("ep", None, "tp"),
        P("ep", "tp", None),
        P(),
        P(None, ("ep", "tp")),
        P(None, ("ep", "tp")),
        P(("ep", "tp"), None),
    )
    return jax.shard_map(
        shards, mesh=mesh, in_specs=placed, out_specs=P("ep", "tp"), check_vma=False
    )
```
